32 devices in a mesh: sp: 8 (over y, x, core), tp: 4 (over z).
Axes of the slice: x: 2, y: 2, z: 4, core: 2. Of those that a mesh axis runs over, the one named last changes fastest.
Arguments:
- sequence: bfloat16 [4, 256, 1024], P(None, 'sp', 'tp'), may hold values from -6 to 6
- norm_gain: float32 [3, 1024], replicated, may hold values from 0.1 to 1.9
- weight_value: bfloat16 [3, 1024, 512], P(None, 'sp', 'tp'), may hold values from -0.1875 to 0.1875
- weight_outer: bfloat16 [3, 1024, 512], P(None, 'sp', 'tp'), may hold values from -0.1875 to 0.1875
- weight_inner: bfloat16 [3, 1024, 512], P(None, 'sp', 'tp'), may hold values from -0.1875 to 0.1875
- conv_taps: float32 [3, 3, 512], P(None, None, 'tp'), may hold values from -3 to 3
- weight_out: bfloat16 [3, 512, 1024], P(None, 'tp', 'sp'), may hold values from -0.25 to 0.25
Outputs:
- mixed: bfloat16 [4, 256, 1024], P(None, 'sp', 'tp')
The draws below stay inside these ranges and needn't reach their ends.
All inputs are finite; a program needn't handle non-finite values.
Results may differ from the reference program's by a relative error of at most 0.03.
Values may be sent and summed in bfloat16 or wider, within the bound.
A program may use at most 64 MiB of HBM per device.

```python
import jax
import jax.numpy as jnp
from jax import lax

D = 1024
CW = 512
KTAPS = 3
LAYERS = 3
SEQS = 4
TOKENS = 256


def level_of(stream_key, extent, shards, smallest, largest):
    def one(position, parts):
        heights = jax.random.uniform(jax.random.fold_in(jax.random.fold_in(stream_key, 6), position), (parts,), jnp.float32, smallest / len(shards), largest / len(shards))
        return jnp.repeat(jnp.exp(heights), extent[position] // parts).reshape((-1,) + (1,) * (len(extent) - position - 1))

    gain = one(*shards[0])
    for cut in shards[1:]:
        gain = gain * one(*cut)
    return gain


def noise(rng, shape, deviation, bound, cuts=(), dtype=jnp.bfloat16):
    level = level_of(rng, shape, cuts, -0.22, 0.18) if cuts else 1.0
    entries = jax.random.normal(rng, shape, jnp.float32) * deviation * level
    return jnp.minimum(jnp.maximum(entries, -bound), bound).astype(dtype)


def setup_inputs(seed: int = 0) -> dict:
    seeds = jax.random.split(jax.random.key(seed), 8)
    sequence = noise(seeds[0], (SEQS, TOKENS, D), 1.0, 6.0, ((1, 8), (2, 4)))
    norm_gain = jnp.clip(1.0 + 0.18 * jax.random.normal(seeds[1], (LAYERS, D), jnp.float32), 0.1, 1.9)
    weight_value = noise(seeds[2], (LAYERS, D, CW), D ** -0.5, 0.1875, ((1, 8), (2, 4)))
    weight_outer = noise(seeds[3], (LAYERS, D, CW), D ** -0.5, 0.1875, ((1, 8), (2, 4)))
    weight_inner = noise(seeds[4], (LAYERS, D, CW), D ** -0.5, 0.1875, ((1, 8), (2, 4)))
    conv_taps = noise(seeds[5], (LAYERS, KTAPS, CW), 0.6, 3.0, ((2, 4),), jnp.float32)
    weight_out = noise(seeds[6], (LAYERS, CW, D), CW ** -0.5, 0.25, ((1, 4), (2, 8)))
    return {"sequence": sequence, "norm_gain": norm_gain, "weight_value": weight_value, "weight_outer": weight_outer, "weight_inner": weight_inner, "conv_taps": conv_taps, "weight_out": weight_out}


def rms_rows(values, gain_row):
    wide = values.astype(jnp.float32)
    scaled = wide * lax.rsqrt(lax.optimization_barrier(jnp.mean(wide * wide, axis=-1, keepdims=True)) + 1e-06)
    return (scaled * gain_row).astype(jnp.bfloat16)

def reference(sequence, norm_gain, weight_value, weight_outer, weight_inner, conv_taps, weight_out):
    current = sequence
    for layer_index in range(LAYERS):
        normed = rms_rows(current, norm_gain[layer_index]).reshape(SEQS * TOKENS, D)
        proj_value = jnp.dot(normed, weight_value[layer_index], preferred_element_type=jnp.float32).astype(jnp.bfloat16)
        proj_outer = jnp.dot(normed, weight_outer[layer_index], preferred_element_type=jnp.float32).astype(jnp.bfloat16)
        proj_inner = jnp.dot(normed, weight_inner[layer_index], preferred_element_type=jnp.float32).astype(jnp.bfloat16)
        product = (proj_inner.astype(jnp.float32) * proj_value.astype(jnp.float32)).reshape(SEQS, TOKENS, CW)
        padded = jnp.pad(product, ((0, 0), (KTAPS - 1, 0), (0, 0)))
        filtered = conv_taps[layer_index, 0] * padded[:, 0:TOKENS]
        for offset in range(1, KTAPS):
            filtered = filtered + conv_taps[layer_index, offset] * padded[:, offset:offset + TOKENS]
        gated = (proj_outer.astype(jnp.float32).reshape(SEQS, TOKENS, CW) * filtered).astype(jnp.bfloat16)
        projected = jnp.dot(gated.reshape(SEQS * TOKENS, CW), weight_out[layer_index], preferred_element_type=jnp.float32)
        current = (current.astype(jnp.float32) + projected.reshape(SEQS, TOKENS, D)).astype(jnp.bfloat16)
    return current
```

```python
import functools

import jax
import jax.numpy as jnp
from jax import lax
from jax.experimental import pallas as pl
from jax.experimental.pallas import tpu as pltpu
from jax.sharding import PartitionSpec as P

LAYERS = 3


def folded(array, axis, dim, update, carry):
    whole = jax.tree.map(lambda part: lax.all_gather(part, axis, axis=dim, tiled=True), array)
    return update(carry, whole, jnp.int32(0))


def from_behind(value, axis, steps):
    count = lax.axis_size(axis)
    first, last = max(0, -steps), min(count, count - steps)
    return lax.ppermute(value, axis, [(source, source + steps) for source in range(first, last)])


def over_all(slab, axis, dim, apply):
    everything = lax.all_gather(slab, axis, axis=dim, tiled=True)
    return apply(everything, jnp.int32(0))


def rms_rows(values, gain_row):
    wide = values.astype(jnp.float32)
    scaled = wide * lax.rsqrt(jnp.mean(wide * wide, axis=-1, keepdims=True) + 1e-06)
    return (scaled * gain_row).astype(jnp.bfloat16)


def body(sequence, norm_gain, weight_value, weight_outer, weight_inner, conv_taps, weight_out):
    current = sequence
    seq_count = sequence.shape[0]
    local_len = sequence.shape[1]
    channels = weight_value.shape[2]
    depth = conv_taps.shape[1]
    for layer_index in range(LAYERS):
        whole = lax.all_gather(current, "tp", axis=2, tiled=True)
        normed = rms_rows(whole, norm_gain[layer_index]).reshape(
            seq_count * local_len, whole.shape[2]
        )
        empty = jnp.zeros((normed.shape[0], channels), jnp.float32)

        def add_rows(running, weight_rows, offset):
            columns = lax.dynamic_slice_in_dim(normed, offset, weight_rows.shape[0], 1)
            return running + jnp.dot(columns, weight_rows, preferred_element_type=jnp.float32)

        sum_value = folded(weight_value[layer_index], "sp", 0, add_rows, empty)
        sum_outer = folded(weight_outer[layer_index], "sp", 0, add_rows, empty)
        sum_inner = folded(weight_inner[layer_index], "sp", 0, add_rows, empty)
        proj_value = sum_value.astype(jnp.bfloat16)
        proj_outer = sum_outer.astype(jnp.bfloat16)
        proj_inner = sum_inner.astype(jnp.bfloat16)
        product = (proj_inner.astype(jnp.float32) * proj_value.astype(jnp.float32)).reshape(
            seq_count, local_len, channels
        )
        last_rows = product[:, local_len - (depth - 1) :, :]
        before = from_behind(last_rows, "sp", 1)
        padded = jnp.concatenate([before, product], axis=1)
        filtered = conv_taps[layer_index, 0] * padded[:, 0:local_len]
        for offset in range(1, depth):
            filtered = (
                filtered + conv_taps[layer_index, offset] * padded[:, offset : offset + local_len]
            )
        gated = (
            proj_outer.astype(jnp.float32).reshape(seq_count, local_len, channels) * filtered
        ).astype(jnp.bfloat16)
        gated_rows = gated.reshape(seq_count * local_len, channels)

        def project_columns(weight_cols, offset):
            return jnp.dot(gated_rows, weight_cols, preferred_element_type=jnp.float32)

        terms = over_all(weight_out[layer_index], "sp", 1, project_columns)
        shares = lax.psum_scatter(
            terms.astype(jnp.bfloat16), "tp", scatter_dimension=1, tiled=True
        ).astype(jnp.float32)
        shares = shares.reshape(seq_count, local_len, shares.shape[1])
        current = (current.astype(jnp.float32) + shares).astype(jnp.bfloat16)
    return current


CORES = 2
HALO = 8
HALO_SENT = 16
COPIES = 176
MESH = pl.DeviceIdType.MESH


def kernel(
    sp, tp, seq_ref, gain_ref, value_ref, outer_ref, inner_ref, taps_ref, out_w_ref, mixed_ref,
    main, edge, win, wout, gates, current,
    send_sem, local_sem, seq_sem, edge_sem, win_sem, win_own_sem, win_fwd_sem,
    rows_sem, wout_sem, wout_own_sem, wout_fwd_sem, gate_sem,
):
    s, t = lax.axis_index("sp"), lax.axis_index("tp")
    chips = sp // CORES
    chip, core = s // CORES, s % CORES
    partner = chip * CORES + (CORES - 1 - core)
    seqs, length, feats = seq_ref.shape
    layers, depth_w, channels = value_ref.shape
    taps = taps_ref.shape[1]
    rows = seqs * (HALO + length)
    width = feats * tp
    sources = (value_ref, outer_ref, inner_ref)
    sends, locals_ = [], []

    def at(sp_index, tp_index):
        return {"sp": sp_index, "tp": tp_index}

    def along(step):
        return lax.rem(t + step + tp, tp)

    def peer(step):
        return lax.rem(chip + step + chips, chips) * CORES + core

    def remote(src, dst, recv, device):
        copy = pltpu.make_async_remote_copy(
            src_ref=src, dst_ref=dst, send_sem=send_sem.at[len(sends)], recv_sem=recv,
            device_id=device, device_id_type=MESH,
        )
        copy.start()
        sends.append(copy)

    def arrived(dst, recv):
        pltpu.make_async_remote_copy(
            src_ref=dst, dst_ref=dst, send_sem=send_sem.at[0], recv_sem=recv,
            device_id=at(partner, t), device_id_type=MESH,
        ).wait_recv()

    def local(src, dst):
        copy = pltpu.make_async_copy(src, dst, local_sem.at[len(locals_)])
        copy.start()
        locals_.append(copy)
        return copy

    right, left = lax.rem(s + 1, sp), lax.rem(s + sp - 1, sp)
    greeted = [at(s, along(step)) for step in range(1, tp)]
    greeted += [at(peer(step), t) for step in range(1, chips)]
    greeted += [at(partner, t)]
    greeted += [at(side, along(step)) for side in (left, right) for step in range(tp)]
    barrier = pltpu.get_barrier_semaphore()
    for device in greeted:
        pl.semaphore_signal(barrier, inc=1, device_id=device, device_id_type=MESH)
    own_main = local(seq_ref, main.at[t])
    own_in = [[local(ref.at[l], win.at[l, s, k]) for k, ref in enumerate(sources)] for l in range(layers)]
    own_out = [local(out_w_ref.at[l], wout.at[l, s, t]) for l in range(layers)]
    pl.semaphore_wait(barrier, len(greeted))

    def send_in(l):
        for k, ref in enumerate(sources):
            for step in range(1, chips):
                remote(ref.at[l], win.at[l, s, k], win_sem.at[l, step, k], at(peer(step), t))
            remote(ref.at[l], win.at[l, s, k], win_own_sem.at[l, k], at(partner, t))

    def send_rows(l):
        for step in range(1, tp):
            remote(out_w_ref.at[l], wout.at[l, s, t], rows_sem.at[l, step], at(s, along(step)))

    def forward_in(l):
        for step in range(1, chips):
            origin = peer(-step)
            for k in range(len(sources)):
                arrived(win.at[l, origin, k], win_sem.at[l, step, k])
            remote(win.at[l, origin], win.at[l, origin], win_fwd_sem.at[l, step], at(partner, t))

    def spread_out(l):
        own_out[l].wait()
        for step in range(1, tp):
            arrived(wout.at[l, s, along(-step)], rows_sem.at[l, step])
        for step in range(1, chips):
            remote(wout.at[l, s], wout.at[l, s], wout_sem.at[l, step], at(peer(step), t))
        remote(wout.at[l, s], wout.at[l, s], wout_own_sem.at[l], at(partner, t))

    def forward_out(l):
        for step in range(1, chips):
            origin = peer(-step)
            arrived(wout.at[l, origin], wout_sem.at[l, step])
            remote(wout.at[l, origin], wout.at[l, origin], wout_fwd_sem.at[l, step], at(partner, t))

    def finish_in(l):
        for copy in own_in[l]:
            copy.wait()
        for k in range(len(sources)):
            arrived(win.at[l, partner, k], win_own_sem.at[l, k])
        for step in range(1, chips):
            origin = lax.rem(chip - step + chips, chips) * CORES + (CORES - 1 - core)
            arrived(win.at[l, origin], win_fwd_sem.at[l, step])

    def finish_out(l):
        arrived(wout.at[l, partner], wout_own_sem.at[l])
        for step in range(1, chips):
            origin = lax.rem(chip - step + chips, chips) * CORES + (CORES - 1 - core)
            arrived(wout.at[l, origin], wout_fwd_sem.at[l, step])

    def gate_layer(l):
        wide = current[...]
        scaled = wide * lax.rsqrt(jnp.mean(wide * wide, axis=-1, keepdims=True) + 1e-06)
        normed = (scaled * gain_ref[l : l + 1, :]).astype(jnp.bfloat16)
        finish_in(l)
        weights = jnp.concatenate(
            [win[l, :, k].reshape(width, channels) for k in range(len(sources))], axis=1
        )
        proj = jnp.dot(normed, weights, preferred_element_type=jnp.float32)
        proj = proj.astype(jnp.bfloat16).astype(jnp.float32)
        product = proj[:, 2 * channels :] * proj[:, :channels]
        filtered = taps_ref[l, taps - 1 : taps, :] * product
        for back in range(1, taps):
            shifted = jnp.concatenate(
                [jnp.zeros((back, channels), jnp.float32), product[: rows - back]], axis=0
            )
            filtered = filtered + taps_ref[l, taps - 1 - back : taps - back, :] * shifted
        gates[l, t] = (proj[:, channels : 2 * channels] * filtered).astype(jnp.bfloat16)
        for step in range(1, tp):
            remote(gates.at[l, t], gates.at[l, t], gate_sem.at[l, step], at(s, along(step)))

    def all_gates(l):
        for step in range(1, tp):
            arrived(gates.at[l, along(-step)], gate_sem.at[l, step])
        return jnp.concatenate([gates[l, j] for j in range(tp)], axis=1)

    for step in range(1, tp):
        remote(seq_ref, main.at[t], seq_sem.at[step], at(s, along(step)))
    for step in range(tp):
        remote(
            seq_ref.at[:, pl.ds(length - HALO_SENT, HALO_SENT), :], edge.at[t], edge_sem.at[step],
            at(right, along(step)),
        )
    send_in(0)
    for l in range(layers):
        send_rows(l)
    send_in(1)
    forward_in(0)
    spread_out(0)
    own_main.wait()
    for step in range(1, tp):
        arrived(main.at[along(-step)], seq_sem.at[step])
    for step in range(tp):
        arrived(edge.at[along(-step)], edge_sem.at[step])
    inside = jnp.where(s == 0, 0.0, 1.0).astype(jnp.float32)
    for j in range(tp):
        before = edge[j].astype(jnp.float32)[:, HALO_SENT - HALO :, :] * inside
        both = jnp.concatenate([before, main[j].astype(jnp.float32)], axis=1)
        current[:, j * feats : (j + 1) * feats] = both.reshape(rows, feats)

    per_dot = 2
    for l in range(layers):
        gate_layer(l)
        if l + 2 < layers:
            send_in(l + 2)
        if l + 1 < layers:
            forward_in(l + 1)
            spread_out(l + 1)
        forward_out(l)
        gated = all_gates(l)
        finish_out(l)

        def columns(first):
            return jnp.concatenate(
                [wout[l, first + j].reshape(tp * channels, depth_w) for j in range(per_dot)], axis=1
            )

        if l < layers - 1:
            for first in range(0, sp, per_dot):
                span = slice(first * depth_w, (first + per_dot) * depth_w)
                added = jnp.dot(gated, columns(first), preferred_element_type=jnp.float32)
                current[:, span] = (current[:, span] + added).astype(jnp.bfloat16).astype(jnp.float32)
        else:
            mine = sp // tp
            for j in range(0, mine, per_dot):
                added = jnp.dot(gated, columns(t * mine + j), preferred_element_type=jnp.float32)
                place = pl.multiple_of(t * feats + j * depth_w, depth_w)
                total = current[:, pl.ds(place, per_dot * depth_w)] + added
                total = total.reshape(seqs, HALO + length, per_dot * depth_w)[:, HALO:, :]
                mixed_ref[:, :, j * depth_w : (j + per_dot) * depth_w] = total.astype(jnp.bfloat16)
    for copy in sends:
        copy.wait_send()


def fused(sp, tp, sequence, norm_gain, weight_value, weight_outer, weight_inner, conv_taps, weight_out):
    seqs, length, feats = sequence.shape
    layers, depth_w, channels = weight_value.shape
    rows = seqs * (HALO + length)
    chips = sp // CORES
    vmem = pl.BlockSpec(memory_space=pltpu.VMEM)
    hbm = pl.BlockSpec(memory_space=pl.ANY)
    dma = pltpu.SemaphoreType.DMA
    return pl.pallas_call(
        functools.partial(kernel, sp, tp),
        out_shape=jax.ShapeDtypeStruct(sequence.shape, sequence.dtype),
        in_specs=[hbm, vmem, hbm, hbm, hbm, vmem, hbm],
        out_specs=vmem,
        scratch_shapes=[
            pltpu.VMEM((tp, seqs, length, feats), jnp.bfloat16),
            pltpu.VMEM((tp, seqs, HALO_SENT, feats), jnp.bfloat16),
            pltpu.VMEM((layers, sp, 3, depth_w, channels), jnp.bfloat16),
            pltpu.VMEM((layers, sp, tp, channels, depth_w), jnp.bfloat16),
            pltpu.VMEM((layers, tp, rows, channels), jnp.bfloat16),
            pltpu.VMEM((rows, feats * tp), jnp.float32),
            dma((COPIES,)),
            dma((1 + 4 * layers,)),
            dma((tp,)),
            dma((tp,)),
            dma((layers, chips, 3)),
            dma((layers, 3)),
            dma((layers, chips)),
            dma((layers, tp)),
            dma((layers, chips)),
            dma((layers,)),
            dma((layers, chips)),
            dma((layers, tp)),
        ],
        compiler_params=pltpu.CompilerParams(collective_id=0, has_side_effects=True),
    )(sequence, norm_gain, weight_value, weight_outer, weight_inner, conv_taps, weight_out)


def fits(sp, tp, sequence, weight_value, conv_taps, weight_out):
    length, feats = sequence.shape[1:]
    depth_w, channels = weight_value.shape[1:]
    reach = conv_taps.shape[0] * (conv_taps.shape[1] - 1)
    aligned = feats % 128 == 0 and depth_w % 128 == 0 and channels % 128 == 0
    shared = sp % (CORES * tp) == 0 and length % 16 == 0 and length >= HALO_SENT
    return aligned and shared and reach <= HALO and weight_out.shape[2] == depth_w


def either(sp, tp, sequence, norm_gain, weight_value, weight_outer, weight_inner, conv_taps, weight_out):
    args = (sequence, norm_gain, weight_value, weight_outer, weight_inner, conv_taps, weight_out)
    if fits(sp, tp, sequence, weight_value, conv_taps, weight_out):
        return fused(sp, tp, *args)
    return body(*args)


def solution(mesh):
    return jax.shard_map(
        functools.partial(either, mesh.shape["sp"], mesh.shape["tp"]),
        mesh=mesh,
        in_specs=(
            P(None, "sp", "tp"),
            P(),
            P(None, "sp", "tp"),
            P(None, "sp", "tp"),
            P(None, "sp", "tp"),
            P(None, None, "tp"),
            P(None, "tp", "sp"),
        ),
        out_specs=P(None, "sp", "tp"),
        check_vma=False,
    )
```

```python
import functools

import jax
import jax.numpy as jnp
from jax import lax
from jax.experimental import pallas as pl
from jax.experimental.pallas import tpu as pltpu
from jax.sharding import PartitionSpec as P

LAYERS = 3


def folded(array, axis, dim, update, carry):
    whole = jax.tree.map(lambda part: lax.all_gather(part, axis, axis=dim, tiled=True), array)
    return update(carry, whole, jnp.int32(0))


def from_behind(value, axis, steps):
    count = lax.axis_size(axis)
    first, last = max(0, -steps), min(count, count - steps)
    return lax.ppermute(value, axis, [(source, source + steps) for source in range(first, last)])


def over_all(slab, axis, dim, apply):
    everything = lax.all_gather(slab, axis, axis=dim, tiled=True)
    return apply(everything, jnp.int32(0))


def rms_rows(values, gain_row):
    wide = values.astype(jnp.float32)
    scaled = wide * lax.rsqrt(jnp.mean(wide * wide, axis=-1, keepdims=True) + 1e-06)
    return (scaled * gain_row).astype(jnp.bfloat16)


def body(sequence, norm_gain, weight_value, weight_outer, weight_inner, conv_taps, weight_out):
    current = sequence
    seq_count = sequence.shape[0]
    local_len = sequence.shape[1]
    channels = weight_value.shape[2]
    depth = conv_taps.shape[1]
    for layer_index in range(LAYERS):
        whole = lax.all_gather(current, "tp", axis=2, tiled=True)
        normed = rms_rows(whole, norm_gain[layer_index]).reshape(
            seq_count * local_len, whole.shape[2]
        )
        empty = jnp.zeros((normed.shape[0], channels), jnp.float32)

        def add_rows(running, weight_rows, offset):
            columns = lax.dynamic_slice_in_dim(normed, offset, weight_rows.shape[0], 1)
            return running + jnp.dot(columns, weight_rows, preferred_element_type=jnp.float32)

        sum_value = folded(weight_value[layer_index], "sp", 0, add_rows, empty)
        sum_outer = folded(weight_outer[layer_index], "sp", 0, add_rows, empty)
        sum_inner = folded(weight_inner[layer_index], "sp", 0, add_rows, empty)
        proj_value = sum_value.astype(jnp.bfloat16)
        proj_outer = sum_outer.astype(jnp.bfloat16)
        proj_inner = sum_inner.astype(jnp.bfloat16)
        product = (proj_inner.astype(jnp.float32) * proj_value.astype(jnp.float32)).reshape(
            seq_count, local_len, channels
        )
        last_rows = product[:, local_len - (depth - 1) :, :]
        before = from_behind(last_rows, "sp", 1)
        padded = jnp.concatenate([before, product], axis=1)
        filtered = conv_taps[layer_index, 0] * padded[:, 0:local_len]
        for offset in range(1, depth):
            filtered = (
                filtered + conv_taps[layer_index, offset] * padded[:, offset : offset + local_len]
            )
        gated = (
            proj_outer.astype(jnp.float32).reshape(seq_count, local_len, channels) * filtered
        ).astype(jnp.bfloat16)
        gated_rows = gated.reshape(seq_count * local_len, channels)

        def project_columns(weight_cols, offset):
            return jnp.dot(gated_rows, weight_cols, preferred_element_type=jnp.float32)

        terms = over_all(weight_out[layer_index], "sp", 1, project_columns)
        shares = lax.psum_scatter(
            terms.astype(jnp.bfloat16), "tp", scatter_dimension=1, tiled=True
        ).astype(jnp.float32)
        shares = shares.reshape(seq_count, local_len, shares.shape[1])
        current = (current.astype(jnp.float32) + shares).astype(jnp.bfloat16)
    return current


CORES = 2
HALO = 8
HALO_SENT = 16
COPIES = 176
MESH = pl.DeviceIdType.MESH


def kernel(
    sp, tp, seq_ref, gain_ref, value_ref, outer_ref, inner_ref, taps_ref, out_w_ref, mixed_ref,
    main, edge, win, wout, gates, current,
    send_sem, local_sem, seq_sem, edge_sem, win_sem, win_own_sem, win_fwd_sem,
    rows_sem, wout_sem, wout_own_sem, wout_fwd_sem, gate_sem,
):
    s, t = lax.axis_index("sp"), lax.axis_index("tp")
    chips = sp // CORES
    chip, core = s // CORES, s % CORES
    partner = chip * CORES + (CORES - 1 - core)
    seqs, length, feats = seq_ref.shape
    layers, depth_w, channels = value_ref.shape
    taps = taps_ref.shape[1]
    rows = seqs * (HALO + length)
    width = feats * tp
    sources = (value_ref, outer_ref, inner_ref)
    sends, locals_ = [], []
    mine = sp // tp
    goal = s // mine

    def wanted(l, device):
        return None if l < layers - 1 else device // mine == t

    def only(condition, act):
        if condition is None:
            act()
        else:
            pl.when(condition)(act)

    def at(sp_index, tp_index):
        return {"sp": sp_index, "tp": tp_index}

    def along(step):
        return lax.rem(t + step + tp, tp)

    def peer(step):
        return lax.rem(chip + step + chips, chips) * CORES + core

    def remote(src, dst, recv, device, condition=None):
        copy = pltpu.make_async_remote_copy(
            src_ref=src, dst_ref=dst, send_sem=send_sem.at[len(sends)], recv_sem=recv,
            device_id=device, device_id_type=MESH,
        )
        only(condition, copy.start)
        sends.append((condition, copy))

    def arrived(dst, recv, condition=None):
        copy = pltpu.make_async_remote_copy(
            src_ref=dst, dst_ref=dst, send_sem=send_sem.at[0], recv_sem=recv,
            device_id=at(partner, t), device_id_type=MESH,
        )
        only(condition, copy.wait_recv)

    def local(src, dst):
        copy = pltpu.make_async_copy(src, dst, local_sem.at[len(locals_)])
        copy.start()
        locals_.append(copy)
        return copy

    right, left = lax.rem(s + 1, sp), lax.rem(s + sp - 1, sp)
    greeted = [at(s, along(step)) for step in range(1, tp)]
    greeted += [at(peer(step), t) for step in range(1, chips)]
    greeted += [at(partner, t)]
    greeted += [at(side, along(step)) for side in (left, right) for step in range(tp)]
    barrier = pltpu.get_barrier_semaphore()
    for device in greeted:
        pl.semaphore_signal(barrier, inc=1, device_id=device, device_id_type=MESH)
    own_main = local(seq_ref, main.at[t])
    own_in = [[local(ref.at[l], win.at[l, s, k]) for k, ref in enumerate(sources)] for l in range(layers)]
    own_out = [local(out_w_ref.at[l], wout.at[l, s, t]) for l in range(layers)]
    pl.semaphore_wait(barrier, len(greeted))

    def send_in(l):
        for k, ref in enumerate(sources):
            for step in range(1, chips):
                remote(ref.at[l], win.at[l, s, k], win_sem.at[l, step, k], at(peer(step), t))
            remote(ref.at[l], win.at[l, s, k], win_own_sem.at[l, k], at(partner, t))

    def send_rows(l):
        for step in range(1, tp):
            condition = None if l < layers - 1 else along(step) == goal
            remote(
                out_w_ref.at[l], wout.at[l, s, t], rows_sem.at[l, step], at(s, along(step)), condition
            )

    def forward_in(l):
        for step in range(1, chips):
            origin = peer(-step)
            for k in range(len(sources)):
                arrived(win.at[l, origin, k], win_sem.at[l, step, k])
            remote(win.at[l, origin], win.at[l, origin], win_fwd_sem.at[l, step], at(partner, t))

    def spread_out(l):
        own_out[l].wait()
        for step in range(1, tp):
            arrived(wout.at[l, s, along(-step)], rows_sem.at[l, step], wanted(l, s))
        for step in range(1, chips):
            remote(
                wout.at[l, s], wout.at[l, s], wout_sem.at[l, step], at(peer(step), t), wanted(l, s)
            )
        remote(wout.at[l, s], wout.at[l, s], wout_own_sem.at[l], at(partner, t), wanted(l, s))

    def forward_out(l):
        for step in range(1, chips):
            origin = peer(-step)
            need = wanted(l, origin)
            arrived(wout.at[l, origin], wout_sem.at[l, step], need)
            remote(
                wout.at[l, origin], wout.at[l, origin], wout_fwd_sem.at[l, step], at(partner, t), need
            )

    def finish_in(l):
        for copy in own_in[l]:
            copy.wait()
        for k in range(len(sources)):
            arrived(win.at[l, partner, k], win_own_sem.at[l, k])
        for step in range(1, chips):
            origin = lax.rem(chip - step + chips, chips) * CORES + (CORES - 1 - core)
            arrived(win.at[l, origin], win_fwd_sem.at[l, step])

    def finish_out(l):
        arrived(wout.at[l, partner], wout_own_sem.at[l], wanted(l, partner))
        for step in range(1, chips):
            origin = lax.rem(chip - step + chips, chips) * CORES + (CORES - 1 - core)
            arrived(wout.at[l, origin], wout_fwd_sem.at[l, step], wanted(l, origin))

    def gate_layer(l):
        wide = current[...]
        scaled = wide * lax.rsqrt(jnp.mean(wide * wide, axis=-1, keepdims=True) + 1e-06)
        normed = (scaled * gain_ref[l : l + 1, :]).astype(jnp.bfloat16)
        finish_in(l)
        weights = jnp.concatenate(
            [win[l, :, k].reshape(width, channels) for k in range(len(sources))], axis=1
        )
        proj = jnp.dot(normed, weights, preferred_element_type=jnp.float32)
        proj = proj.astype(jnp.bfloat16).astype(jnp.float32)
        product = proj[:, 2 * channels :] * proj[:, :channels]
        filtered = taps_ref[l, taps - 1 : taps, :] * product
        for back in range(1, taps):
            shifted = jnp.concatenate(
                [jnp.zeros((back, channels), jnp.float32), product[: rows - back]], axis=0
            )
            filtered = filtered + taps_ref[l, taps - 1 - back : taps - back, :] * shifted
        gates[l, t] = (proj[:, channels : 2 * channels] * filtered).astype(jnp.bfloat16)
        for step in range(1, tp):
            remote(gates.at[l, t], gates.at[l, t], gate_sem.at[l, step], at(s, along(step)))

    def all_gates(l):
        for step in range(1, tp):
            arrived(gates.at[l, along(-step)], gate_sem.at[l, step])
        return jnp.concatenate([gates[l, j] for j in range(tp)], axis=1)

    for step in range(1, tp):
        remote(seq_ref, main.at[t], seq_sem.at[step], at(s, along(step)))
    for step in range(tp):
        remote(
            seq_ref.at[:, pl.ds(length - HALO_SENT, HALO_SENT), :], edge.at[t], edge_sem.at[step],
            at(right, along(step)),
        )
    send_in(0)
    for l in range(layers):
        send_rows(l)
    send_in(1)
    forward_in(0)
    spread_out(0)
    own_main.wait()
    for step in range(1, tp):
        arrived(main.at[along(-step)], seq_sem.at[step])
    for step in range(tp):
        arrived(edge.at[along(-step)], edge_sem.at[step])
    inside = jnp.where(s == 0, 0.0, 1.0).astype(jnp.float32)
    for j in range(tp):
        before = edge[j].astype(jnp.float32)[:, HALO_SENT - HALO :, :] * inside
        both = jnp.concatenate([before, main[j].astype(jnp.float32)], axis=1)
        current[:, j * feats : (j + 1) * feats] = both.reshape(rows, feats)

    per_dot = 2
    for l in range(layers):
        gate_layer(l)
        if l == 0:
            for later in range(2, layers):
                send_in(later)
            for later in range(1, layers):
                spread_out(later)
        if l + 1 < layers:
            forward_in(l + 1)
        forward_out(l)
        gated = all_gates(l)
        finish_out(l)

        def columns(first):
            return jnp.concatenate(
                [wout[l, first + j].reshape(tp * channels, depth_w) for j in range(per_dot)], axis=1
            )

        if l < layers - 1:
            for first in range(0, sp, per_dot):
                span = slice(first * depth_w, (first + per_dot) * depth_w)
                added = jnp.dot(gated, columns(first), preferred_element_type=jnp.float32)
                current[:, span] = (current[:, span] + added).astype(jnp.bfloat16).astype(jnp.float32)
        else:
            mine = sp // tp
            for j in range(0, mine, per_dot):
                added = jnp.dot(gated, columns(t * mine + j), preferred_element_type=jnp.float32)
                place = pl.multiple_of(t * feats + j * depth_w, depth_w)
                total = current[:, pl.ds(place, per_dot * depth_w)] + added
                total = total.reshape(seqs, HALO + length, per_dot * depth_w)[:, HALO:, :]
                mixed_ref[:, :, j * depth_w : (j + per_dot) * depth_w] = total.astype(jnp.bfloat16)
    for condition, copy in sends:
        only(condition, copy.wait_send)


def fused(sp, tp, sequence, norm_gain, weight_value, weight_outer, weight_inner, conv_taps, weight_out):
    seqs, length, feats = sequence.shape
    layers, depth_w, channels = weight_value.shape
    rows = seqs * (HALO + length)
    chips = sp // CORES
    vmem = pl.BlockSpec(memory_space=pltpu.VMEM)
    hbm = pl.BlockSpec(memory_space=pl.ANY)
    dma = pltpu.SemaphoreType.DMA
    return pl.pallas_call(
        functools.partial(kernel, sp, tp),
        out_shape=jax.ShapeDtypeStruct(sequence.shape, sequence.dtype),
        in_specs=[hbm, vmem, hbm, hbm, hbm, vmem, hbm],
        out_specs=vmem,
        scratch_shapes=[
            pltpu.VMEM((tp, seqs, length, feats), jnp.bfloat16),
            pltpu.VMEM((tp, seqs, HALO_SENT, feats), jnp.bfloat16),
            pltpu.VMEM((layers, sp, 3, depth_w, channels), jnp.bfloat16),
            pltpu.VMEM((layers, sp, tp, channels, depth_w), jnp.bfloat16),
            pltpu.VMEM((layers, tp, rows, channels), jnp.bfloat16),
            pltpu.VMEM((rows, feats * tp), jnp.float32),
            dma((COPIES,)),
            dma((1 + 4 * layers,)),
            dma((tp,)),
            dma((tp,)),
            dma((layers, chips, 3)),
            dma((layers, 3)),
            dma((layers, chips)),
            dma((layers, tp)),
            dma((layers, chips)),
            dma((layers,)),
            dma((layers, chips)),
            dma((layers, tp)),
        ],
        compiler_params=pltpu.CompilerParams(collective_id=0, has_side_effects=True),
    )(sequence, norm_gain, weight_value, weight_outer, weight_inner, conv_taps, weight_out)


def fits(sp, tp, sequence, weight_value, conv_taps, weight_out):
    length, feats = sequence.shape[1:]
    depth_w, channels = weight_value.shape[1:]
    reach = conv_taps.shape[0] * (conv_taps.shape[1] - 1)
    aligned = feats % 128 == 0 and depth_w % 128 == 0 and channels % 128 == 0
    shared = sp % (CORES * tp) == 0 and length % 16 == 0 and length >= HALO_SENT
    return aligned and shared and reach <= HALO and weight_out.shape[2] == depth_w


def either(sp, tp, sequence, norm_gain, weight_value, weight_outer, weight_inner, conv_taps, weight_out):
    args = (sequence, norm_gain, weight_value, weight_outer, weight_inner, conv_taps, weight_out)
    if fits(sp, tp, sequence, weight_value, conv_taps, weight_out):
        return fused(sp, tp, *args)
    return body(*args)


def solution(mesh):
    return jax.shard_map(
        functools.partial(either, mesh.shape["sp"], mesh.shape["tp"]),
        mesh=mesh,
        in_specs=(
            P(None, "sp", "tp"),
            P(),
            P(None, "sp", "tp"),
            P(None, "sp", "tp"),
            P(None, "sp", "tp"),
            P(None, None, "tp"),
            P(None, "tp", "sp"),
        ),
        out_specs=P(None, "sp", "tp"),
        check_vma=False,
    )
```
